32 devices in a mesh: kv: 8 (over z, x), tp: 4 (over y, core).
Axes of the slice: x: 2, y: 2, z: 4, core: 2. Of those that a mesh axis runs over, the one named last changes fastest.
Arguments:
- tokens: bfloat16 [4, 4096], P(None, 'kv'), may hold values from -30 to 30
- norm_gain: float32 [4096], P('kv'), may hold values from 0.1 to 1.9
- query_weight: bfloat16 [4096, 2048], P('kv', 'tp'), may hold values from -0.09375 to 0.09375
- cache_keys: bfloat16 [4, 4096, 16, 128], P(None, 'kv', 'tp'), may hold values from -180 to 180
- cache_values: bfloat16 [4, 4096, 16, 128], P(None, 'kv', 'tp'), may hold values from -6 to 6
- lengths: int32 [4], replicated, may hold values from 2049 to 4096, as said below
- lambdas: float32 [16], P('tp'), may hold values from 0.3 to 0.8
- head_gain: float32 [128], replicated, may hold values from 0.1 to 1.9
- out_weight: bfloat16 [2048, 4096], P('tp', 'kv'), may hold values from -0.125 to 0.125
Outputs:
- mixed: bfloat16 [4, 4096], P(None, 'kv')
The draws below stay inside these ranges and needn't reach their ends.
Inputs may be any that keep to these rules, and one draw needn't show every extreme that they name: `lengths`: every length is more than half of 4096; some sequence has exactly 4096.
All inputs are finite; a program needn't handle non-finite values.
Results may differ from the reference program's by a relative error of at most 0.02.
Values may be sent and summed in bfloat16 or wider, within the bound.
No kernel may reach another device: no remote copies, remote signals or barrier semaphores. Data moves between devices by JAX's collectives and lax.ppermute only.
A program may use at most 64 MiB of HBM per device.

```python
import math
import jax
import jax.numpy as jnp
from jax import lax

D = 4096
HEADS = 16
HD = 64
VD = 128
SEQS = 4
LENGTH = 4096
N_TP = 4


def draw_tokens(key, part):
    first = jax.random.fold_in(jax.random.fold_in(key, 11), 0)
    second = jax.random.fold_in(jax.random.fold_in(key, 11), 1)
    fourth = jax.random.fold_in(jax.random.fold_in(key, 11), 3)
    column = jnp.arange(D, dtype=jnp.int32)
    phase = jax.random.uniform(first, (), jnp.float32, 0.0, 2.0 * math.pi)
    blocks = jnp.exp(jax.random.uniform(second, (D // 32,), jnp.float32, math.log(0.6), math.log(1.7)))
    scale = jnp.exp(1.2 * jnp.sin(2.0 * math.pi * column.astype(jnp.float32) / D + phase)) * blocks[column // 32]
    base = jnp.clip(jax.random.normal(fourth, (SEQS, D), jnp.float32), -4.5, 4.5)
    return (base * scale[None, :]).astype(jnp.bfloat16)


def draw_cache_keys(key, part):
    key_drawn = jax.random.fold_in(jax.random.fold_in(key, 23), 4)
    shape = (SEQS, LENGTH, HEADS, 2 * HD)
    base = jnp.clip(1.75 * jax.random.normal(key_drawn, shape, jnp.float32), -7.0, 7.0)
    return base.astype(jnp.bfloat16)


def draw_lengths(key, part):
    first, second = jax.random.split(jax.random.fold_in(key, 37))
    value_rows = jax.random.randint(first, (SEQS,), LENGTH // 2 + 1, LENGTH + 1)
    chosen = jax.random.randint(second, (), 0, SEQS)
    return jnp.where(jnp.arange(SEQS, dtype=jnp.int32) == chosen, LENGTH, value_rows).astype(jnp.int32)


def block_levels(rng, shape, cuts, low, top_value):
    level, own = 1.0, jax.random.fold_in(rng, 6)
    for position, parts in cuts:
        heights = jnp.exp(jax.random.uniform(jax.random.fold_in(own, position), (parts,), jnp.float32, low / len(cuts), top_value / len(cuts)))
        level = level * jnp.repeat(heights, shape[position] // parts).reshape([-1 if axis == position else 1 for axis in range(len(shape))])
    return level


def scatter_about(key, shape, width, limit, cuts=(), held_as=jnp.bfloat16):
    array = width * jax.random.normal(key, shape, jnp.float32)
    if cuts:
        array = array * block_levels(key, shape, cuts, -0.22, 0.18)
    return jnp.clip(array, -limit, limit).astype(held_as)


def setup_inputs(seed: int = 0) -> dict:
    splits = jax.random.split(jax.random.key(seed), 10)
    tokens = draw_tokens(jax.random.fold_in(splits[9], 71), 0)
    norm_gain = jnp.clip(1.0 + 0.18 * jax.random.normal(splits[1], (D,), jnp.float32), 0.1, 1.9)
    query_weight = scatter_about(splits[2], (D, HEADS * 2 * HD), D ** -0.5, 0.09375, ((0, 8), (1, 4)))
    cache_keys = draw_cache_keys(jax.random.fold_in(splits[9], 71), 0)
    cache_values = scatter_about(splits[4], (SEQS, LENGTH, HEADS, VD), 1.0, 6.0, ((1, 8), (2, 4)))
    lengths = draw_lengths(jax.random.fold_in(splits[9], 71), 0)
    lambdas = jnp.clip(0.3 + 0.5 * jax.random.uniform(splits[6], (HEADS,), jnp.float32) ** block_levels(splits[6], (HEADS,), ((0, 4),), -0.2, 0.2), 0.3, 0.8)
    head_gain = jnp.clip(1.0 + 0.18 * jax.random.normal(splits[7], (VD,), jnp.float32), 0.1, 1.9)
    out_weight = scatter_about(splits[8], (HEADS * VD, D), (HEADS * VD) ** -0.5, 0.125, ((0, 4), (1, 8)))
    return {"tokens": tokens, "norm_gain": norm_gain, "query_weight": query_weight, "cache_keys": cache_keys, "cache_values": cache_values, "lengths": lengths, "lambdas": lambdas, "head_gain": head_gain, "out_weight": out_weight}


eps = 1e-06
NEG = -1e+30

def reference(tokens, norm_gain, query_weight, cache_keys, cache_values, lengths, lambdas, head_gain, out_weight):
    floats = tokens.astype(jnp.float32)
    squares = lax.optimization_barrier(jnp.sum(floats * floats, axis=1))
    scaled_logits = (floats * norm_gain).astype(jnp.bfloat16)
    projected = jnp.dot(scaled_logits, query_weight, preferred_element_type=jnp.float32)
    inverse = lax.rsqrt(squares / D + eps)
    query = (projected * inverse[:, None] * 0.125).astype(jnp.bfloat16).reshape(SEQS, HEADS, 2, HD)
    keys = cache_keys.reshape(SEQS, LENGTH, HEADS, 2, HD)

    def one_sequence(args):
        query_row, key_rows_block, vrows, length = args
        score_matrix = jnp.einsum('yvn,wyvn->yvw', query_row.astype(jnp.float32), key_rows_block.astype(jnp.float32))
        valid = (jnp.arange(LENGTH, dtype=jnp.int32) < length)[None, None, :]
        score_matrix = jnp.where(valid, score_matrix, NEG)
        peak = lax.optimization_barrier(jnp.max(score_matrix, axis=-1, keepdims=True))
        weights = jnp.where(valid, jnp.exp(score_matrix - peak), 0.0)
        mass = lax.optimization_barrier(jnp.sum(weights, axis=-1))
        rounded = lax.optimization_barrier(weights.astype(jnp.bfloat16)).astype(jnp.float32)
        summed = jnp.einsum('hmp,phv->hmv', rounded, vrows.astype(jnp.float32))
        return summed / mass[..., None]
    ratios = lax.map(one_sequence, (query, keys, cache_values, lengths))
    attended = ratios[:, :, 0] - lambdas[None, :, None] * ratios[:, :, 1]
    normed = attended * lax.rsqrt(lax.optimization_barrier(jnp.mean(attended * attended, axis=-1, keepdims=True)) + eps) * head_gain * 0.8
    normed = normed.astype(jnp.bfloat16).reshape(SEQS, HEADS * VD)
    rows = HEADS * VD // N_TP
    total = jnp.zeros((SEQS, D), jnp.float32)
    for group in range(N_TP):
        part = jnp.dot(normed[:, group * rows:(group + 1) * rows], out_weight[group * rows:(group + 1) * rows], preferred_element_type=jnp.float32).astype(jnp.bfloat16)
        total = total + part.astype(jnp.float32)
    return total.astype(jnp.bfloat16)
```

```python
import functools

import jax
import jax.numpy as jnp
from jax import lax
from jax.experimental import pallas as pl
from jax.experimental.pallas import tpu as pltpu
from jax.sharding import PartitionSpec as P

EPS = 1e-06
NEG = -1e30
LANES = 128
SUBLANES = 8


VMEM = pltpu.VMEM
SMEM = pltpu.SMEM


def up(n, k):
    return -(-n // k) * k


def project_kernel(tokens_ref, gain_ref, weight_ref, out_ref):
    seqs = tokens_ref.shape[0]
    heads = weight_ref.shape[1] // LANES
    floats = tokens_ref[...].astype(jnp.float32)
    scaled = (floats * gain_ref[...]).astype(jnp.bfloat16)
    projected = jnp.dot(scaled, weight_ref[...], preferred_element_type=jnp.float32)
    for h in range(heads):
        out_ref[h * seqs : (h + 1) * seqs, :] = projected[:, h * LANES : (h + 1) * LANES]
    squares = jnp.sum(floats * floats, axis=1, keepdims=True)
    out_ref[heads * seqs :, :] = jnp.zeros_like(out_ref[heads * seqs :, :])
    out_ref[heads * seqs : (heads + 1) * seqs, :] = jnp.broadcast_to(squares, (seqs, LANES))


def split3(x):
    high = x.astype(jnp.bfloat16).astype(jnp.float32)
    rest = x - high
    middle = rest.astype(jnp.bfloat16).astype(jnp.float32)
    return high, middle, rest - middle


def attend_kernel(width, seqs, heads, *refs):
    shares = refs[:-6]
    lengths_ref, keys_ref, values_ref, out_ref, query_scr, block_scr = refs[-6:]
    hd = LANES // 2
    rows = 2 * heads
    columns = keys_ref.shape[1]
    span = columns // heads
    whole = shares[0][...]
    for ref in shares[1:]:
        whole = whole + ref[...]
    squares = whole[heads * seqs : (heads + 1) * seqs, :]
    inverse = lax.rsqrt(squares / width + EPS) * 0.125
    for h in range(heads):
        query_scr[h * seqs : (h + 1) * seqs, :] = whole[h * seqs : (h + 1) * seqs, :] * inverse
    base = lax.axis_index("kv") * span
    lane = lax.broadcasted_iota(jnp.int32, (rows, LANES), 1)
    sub = lax.broadcasted_iota(jnp.int32, (rows, LANES), 0)
    column = lax.broadcasted_iota(jnp.int32, (rows, columns), 1)
    row = lax.broadcasted_iota(jnp.int32, (rows, columns), 0)
    mine = lax.rem(column, heads) == lax.rem(row, heads)
    peaks = jnp.zeros((rows, LANES), jnp.float32)
    masses = jnp.zeros((rows, LANES), jnp.float32)
    for s in range(seqs):
        one = query_scr[pl.ds(s, heads, stride=seqs), :]
        both = jnp.concatenate([one, one], axis=0)
        query = jnp.where((lane < hd) == (sub < heads), both, 0.0).astype(jnp.bfloat16)
        scores = lax.dot_general(
            query, keys_ref[s], (((1,), (1,)), ((), ())), preferred_element_type=jnp.float32
        )
        valid = mine & (column < (lengths_ref[s] - base) * heads)
        scores = jnp.where(valid, scores, NEG)
        peak = jnp.max(scores, axis=1, keepdims=True)
        weights = jnp.where(valid, jnp.exp(scores - peak), 0.0)
        mass = jnp.sum(weights, axis=1, keepdims=True)
        block_scr[s * rows : (s + 1) * rows, :] = jnp.dot(
            weights.astype(jnp.bfloat16), values_ref[s], preferred_element_type=jnp.float32
        )
        here = lane == s * rows + sub
        peaks = jnp.where(here, peak, peaks)
        masses = jnp.where(here, mass, masses)
    parts = split3(jnp.sum(peaks, axis=0, keepdims=True)) + split3(jnp.sum(masses, axis=0, keepdims=True))
    total = seqs * rows
    tail = lax.broadcasted_iota(jnp.int32, (SUBLANES, LANES), 0)
    stats = jnp.zeros((SUBLANES, LANES), jnp.float32)
    for i, part in enumerate(parts):
        stats = jnp.where(tail == i, part, stats)
    block_scr[total : total + SUBLANES, :] = stats
    block = block_scr[...].astype(jnp.bfloat16)
    for i in range(out_ref.shape[0]):
        out_ref[i] = block


def combine_kernel(seqs, heads, blocks_ref, lambdas_ref, gain_ref, weight_ref, out_ref, att_scr):
    shards = blocks_ref.shape[0]
    rows = 2 * heads
    total = seqs * rows
    stats = [blocks_ref[:, total + i, :].astype(jnp.float32) for i in range(6)]
    peaks = stats[0] + stats[1] + stats[2]
    masses = stats[3] + stats[4] + stats[5]
    factor = jnp.exp(peaks - jnp.max(peaks, axis=0, keepdims=True))
    mass = jnp.sum(masses * factor, axis=0, keepdims=True)
    lane = lax.broadcasted_iota(jnp.int32, (1, LANES), 1)
    sign = jnp.ones((1, LANES), jnp.float32)
    for h in range(heads):
        sign = jnp.where(lax.rem(lane, rows) == heads + h, -lambdas_ref[h], sign)
    scale = factor * (sign / mass)
    turned = jnp.transpose(scale)
    summed = jnp.zeros((total, LANES), jnp.float32)
    for k in range(shards):
        summed = summed + turned[:total, k : k + 1] * blocks_ref[k, :total, :].astype(jnp.float32)
    for s in range(seqs):
        att = summed[s * rows : s * rows + heads] + summed[s * rows + heads : (s + 1) * rows]
        norm = lax.rsqrt(jnp.mean(att * att, axis=1, keepdims=True) + EPS)
        att_scr[s * heads : (s + 1) * heads, :] = att * norm * gain_ref[...] * 0.8
    part = jnp.zeros(out_ref.shape, jnp.float32)
    for h in range(heads):
        normed = att_scr[pl.ds(h, seqs, stride=heads), :].astype(jnp.bfloat16)
        part = part + jnp.dot(
            normed, weight_ref[h * LANES : (h + 1) * LANES, :], preferred_element_type=jnp.float32
        )
    out_ref[...] = part.astype(jnp.bfloat16)


def near(x):
    return pltpu.with_memory_space_constraint(x, VMEM)


def params(limit):
    return pltpu.CompilerParams(vmem_limit_bytes=limit * 1024 * 1024)


def vspec():
    return pl.BlockSpec(memory_space=VMEM)


def sspec():
    return pl.BlockSpec(memory_space=SMEM)


def rounds_of(n):
    out, low = [], 1
    while low < n:
        if low * 4 <= n:
            out.append([low, 2 * low, 3 * low])
            low *= 4
        else:
            out.append([low])
            low *= 2
    return out[::-1]


def exchanged(x, axis, n, distances):
    return [lax.ppermute(x, axis, [(i, i ^ d) for i in range(n)]) for d in distances]


def shares_of(x, axis, n):
    if n & (n - 1):
        whole = lax.all_to_all(jnp.broadcast_to(x[None], (n,) + x.shape), axis, 0, 0)
        return [jnp.sum(whole, axis=0)]
    rounds = rounds_of(n)
    for i, distances in enumerate(rounds):
        parts = [x] + exchanged(x, axis, n, distances)
        if i == len(rounds) - 1:
            return parts
        x = functools.reduce(jnp.add, parts)
    return [x]


def body(
    n_kv,
    n_tp,
    tokens,
    norm_gain,
    query_weight,
    cache_keys,
    cache_values,
    lengths,
    lambdas,
    head_gain,
    out_weight,
):
    seqs, local = tokens.shape
    width = local * n_kv
    span, heads = cache_keys.shape[1:3]
    keys = near(cache_keys.reshape(seqs, span * heads, LANES))
    values = near(cache_values.reshape(seqs, span * heads, LANES))
    sent_rows = up((heads + 1) * seqs, SUBLANES)
    share = pl.pallas_call(
        project_kernel,
        out_shape=VMEM((sent_rows, LANES), jnp.float32),
        in_specs=[vspec(), vspec(), vspec()],
        out_specs=vspec(),
        compiler_params=params(4),
        name="project",
    )(tokens, norm_gain.reshape(1, local), query_weight)
    shares = shares_of(share, "kv", n_kv)
    total = 2 * heads * seqs
    blocks = pl.pallas_call(
        functools.partial(attend_kernel, width, seqs, heads),
        out_shape=VMEM((n_kv, total + SUBLANES, LANES), jnp.bfloat16),
        in_specs=[vspec()] * len(shares) + [sspec(), vspec(), vspec()],
        out_specs=vspec(),
        scratch_shapes=[
            VMEM((heads * seqs, LANES), jnp.float32),
            VMEM((total + SUBLANES, LANES), jnp.float32),
        ],
        compiler_params=params(16),
        name="attend",
    )(*map(near, shares), lengths, keys, values)
    blocks = lax.all_to_all(blocks, "kv", 0, 0)
    part = pl.pallas_call(
        functools.partial(combine_kernel, seqs, heads),
        out_shape=VMEM((seqs, out_weight.shape[1]), jnp.bfloat16),
        in_specs=[vspec(), sspec(), vspec(), vspec()],
        out_specs=vspec(),
        scratch_shapes=[VMEM((heads * seqs, LANES), jnp.float32)],
        compiler_params=params(8),
        name="combine",
    )(near(blocks), lambdas, near(head_gain.reshape(1, LANES)), near(out_weight))
    if n_tp & (n_tp - 1):
        parts = list(lax.all_gather(part, "tp"))
    else:
        parts = [part] + exchanged(part, "tp", n_tp, range(1, n_tp))
    mixed = functools.reduce(jnp.add, [p.astype(jnp.float32) for p in parts])
    return mixed.astype(jnp.bfloat16)


def solution(mesh):
    in_specs = (
        P(None, "kv"),
        P("kv"),
        P("kv", "tp"),
        P(None, "kv", "tp", None),
        P(None, "kv", "tp", None),
        P(),
        P("tp"),
        P(),
        P("tp", "kv"),
    )
    step = functools.partial(body, mesh.shape["kv"], mesh.shape["tp"])
    return jax.shard_map(step, mesh=mesh, in_specs=in_specs, out_specs=P(None, "kv"), check_vma=False)
```

```python
import functools

import jax
import jax.numpy as jnp
from jax import lax
from jax.experimental import pallas as pl
from jax.experimental.pallas import tpu as pltpu
from jax.sharding import PartitionSpec as P

EPS = 1e-06
NEG = -1e30
LANES = 128
SUBLANES = 8


FLOPS, BYTES = 10**10, 10**8

VMEM = pltpu.VMEM
SMEM = pltpu.SMEM


def up(n, k):
    return -(-n // k) * k


def project_kernel(tokens_hbm, gain_hbm, weight_hbm, out_ref, tokens_ref, gain_ref, weight_ref, sems):
    copies = [
        pltpu.make_async_copy(source, target, sems.at[i])
        for i, (source, target) in enumerate(
            ((weight_hbm, weight_ref), (tokens_hbm, tokens_ref), (gain_hbm, gain_ref))
        )
    ]
    for copy in copies:
        copy.start()
    for copy in copies[::-1]:
        copy.wait()
    seqs = tokens_ref.shape[0]
    heads = weight_ref.shape[1] // LANES
    floats = tokens_ref[...].astype(jnp.float32)
    scaled = (floats * gain_ref[...]).astype(jnp.bfloat16)
    projected = jnp.dot(scaled, weight_ref[...], preferred_element_type=jnp.float32)
    squares = jnp.sum(floats * floats, axis=1, keepdims=True)
    block = [projected[:, h * LANES : (h + 1) * LANES] for h in range(heads)]
    block += [jnp.broadcast_to(squares, (seqs, LANES))]
    pad = out_ref.shape[0] - (heads + 1) * seqs
    if pad:
        block += [jnp.zeros((pad, LANES), jnp.float32)]
    out_ref[...] = jnp.concatenate(block, axis=0)


def spread_kernel(block_ref, out_ref):
    block = block_ref[...]
    for i in range(out_ref.shape[0]):
        out_ref[i] = block


def split3(x):
    high = x.astype(jnp.bfloat16).astype(jnp.float32)
    rest = x - high
    middle = rest.astype(jnp.bfloat16).astype(jnp.float32)
    return high, middle, rest - middle


def attend_kernel(width, seqs, heads, *refs):
    shares_ref, lengths_ref, keys_ref, values_ref, out_ref, query_scr, block_scr = refs
    hd = LANES // 2
    rows = 2 * heads
    columns = keys_ref.shape[1]
    span = columns // heads
    whole = jnp.sum(shares_ref[...], axis=0)
    squares = whole[heads * seqs : (heads + 1) * seqs, :]
    inverse = lax.rsqrt(squares / width + EPS) * 0.125
    for h in range(heads):
        query_scr[h * seqs : (h + 1) * seqs, :] = whole[h * seqs : (h + 1) * seqs, :] * inverse
    base = lax.axis_index("kv") * span
    lane = lax.broadcasted_iota(jnp.int32, (rows, LANES), 1)
    sub = lax.broadcasted_iota(jnp.int32, (rows, LANES), 0)
    column = lax.broadcasted_iota(jnp.int32, (rows, columns), 1)
    row = lax.broadcasted_iota(jnp.int32, (rows, columns), 0)
    mine = lax.rem(column, heads) == lax.rem(row, heads)
    peaks = jnp.zeros((rows, LANES), jnp.float32)
    masses = jnp.zeros((rows, LANES), jnp.float32)
    for s in range(seqs):
        one = query_scr[pl.ds(s, heads, stride=seqs), :]
        both = jnp.concatenate([one, one], axis=0)
        query = jnp.where((lane < hd) == (sub < heads), both, 0.0).astype(jnp.bfloat16)
        scores = lax.dot_general(
            query, keys_ref[s], (((1,), (1,)), ((), ())), preferred_element_type=jnp.float32
        )
        valid = mine & (column < (lengths_ref[s] - base) * heads)
        scores = jnp.where(valid, scores, NEG)
        peak = jnp.max(scores, axis=1, keepdims=True)
        weights = jnp.where(valid, jnp.exp(scores - peak), 0.0)
        mass = jnp.sum(weights, axis=1, keepdims=True)
        block_scr[s * rows : (s + 1) * rows, :] = jnp.dot(
            weights.astype(jnp.bfloat16), values_ref[s], preferred_element_type=jnp.float32
        )
        here = lane == s * rows + sub
        peaks = jnp.where(here, peak, peaks)
        masses = jnp.where(here, mass, masses)
    parts = split3(jnp.sum(peaks, axis=0, keepdims=True)) + split3(jnp.sum(masses, axis=0, keepdims=True))
    total = seqs * rows
    tail = lax.broadcasted_iota(jnp.int32, (SUBLANES, LANES), 0)
    stats = jnp.zeros((SUBLANES, LANES), jnp.float32)
    for i, part in enumerate(parts):
        stats = jnp.where(tail == i, part, stats)
    block_scr[total : total + SUBLANES, :] = stats
    block = block_scr[...].astype(jnp.bfloat16)
    for i in range(out_ref.shape[0]):
        out_ref[i] = block


def combine_kernel(seqs, heads, blocks_ref, lambdas_ref, gain_ref, weight_ref, out_ref, att_scr):
    shards = blocks_ref.shape[0]
    rows = 2 * heads
    total = seqs * rows
    stats = [blocks_ref[:, total + i, :].astype(jnp.float32) for i in range(6)]
    peaks = stats[0] + stats[1] + stats[2]
    masses = stats[3] + stats[4] + stats[5]
    factor = jnp.exp(peaks - jnp.max(peaks, axis=0, keepdims=True))
    mass = jnp.sum(masses * factor, axis=0, keepdims=True)
    lane = lax.broadcasted_iota(jnp.int32, (1, LANES), 1)
    sign = jnp.ones((1, LANES), jnp.float32)
    for h in range(heads):
        sign = jnp.where(lax.rem(lane, rows) == heads + h, -lambdas_ref[h], sign)
    scale = factor * (sign / mass)
    turned = jnp.transpose(scale)
    summed = jnp.zeros((total, LANES), jnp.float32)
    for k in range(shards):
        summed = summed + turned[:total, k : k + 1] * blocks_ref[k, :total, :].astype(jnp.float32)
    for s in range(seqs):
        att = summed[s * rows : s * rows + heads] + summed[s * rows + heads : (s + 1) * rows]
        norm = lax.rsqrt(jnp.mean(att * att, axis=1, keepdims=True) + EPS)
        att_scr[s * heads : (s + 1) * heads, :] = att * norm * gain_ref[...] * 0.8
    part = jnp.zeros(out_ref.shape, jnp.float32)
    for h in range(heads):
        normed = att_scr[pl.ds(h, seqs, stride=heads), :].astype(jnp.bfloat16)
        part = part + jnp.dot(
            normed, weight_ref[h * LANES : (h + 1) * LANES, :], preferred_element_type=jnp.float32
        )
    out_ref[...] = part.astype(jnp.bfloat16)


def far(x):
    return pltpu.with_memory_space_constraint(x, pltpu.HBM)


def near(x):
    return pltpu.with_memory_space_constraint(x, VMEM)


def params(limit):
    return pltpu.CompilerParams(vmem_limit_bytes=limit * 1024 * 1024)


def vspec():
    return pl.BlockSpec(memory_space=VMEM)


def hspec():
    return pl.BlockSpec(memory_space=pltpu.HBM)


def sspec():
    return pl.BlockSpec(memory_space=SMEM)


def exchanged(x, axis, n, distances):
    return [lax.ppermute(x, axis, [(i, i ^ d) for i in range(n)]) for d in distances]


def body(
    n_kv,
    n_tp,
    tokens,
    norm_gain,
    query_weight,
    cache_keys,
    cache_values,
    lengths,
    lambdas,
    head_gain,
    out_weight,
):
    seqs, local = tokens.shape
    width = local * n_kv
    span, heads = cache_keys.shape[1:3]
    keys = near(cache_keys.reshape(seqs, span * heads, LANES))
    values = near(cache_values.reshape(seqs, span * heads, LANES))
    sent_rows = up((heads + 1) * seqs, SUBLANES)
    share = pl.pallas_call(
        project_kernel,
        out_shape=VMEM((sent_rows, LANES), jnp.float32),
        in_specs=[hspec(), hspec(), hspec()],
        out_specs=vspec(),
        scratch_shapes=[
            VMEM((seqs, local), tokens.dtype),
            VMEM((1, local), norm_gain.dtype),
            VMEM(query_weight.shape, query_weight.dtype),
            pltpu.SemaphoreType.DMA((3,)),
        ],
        compiler_params=params(4),
        name="project",
    )(far(tokens), far(norm_gain.reshape(1, local)), far(query_weight))
    spread = pl.pallas_call(
        spread_kernel,
        out_shape=VMEM((n_kv,) + share.shape, share.dtype),
        in_specs=[vspec()],
        out_specs=vspec(),
        compiler_params=params(4),
        cost_estimate=pl.CostEstimate(flops=FLOPS, bytes_accessed=BYTES, transcendentals=0),
        name="spread",
    )(near(share))
    shares = lax.all_to_all(spread, "kv", 0, 0)
    total = 2 * heads * seqs
    blocks = pl.pallas_call(
        functools.partial(attend_kernel, width, seqs, heads),
        out_shape=VMEM((n_kv, total + SUBLANES, LANES), jnp.bfloat16),
        in_specs=[vspec(), sspec(), vspec(), vspec()],
        out_specs=vspec(),
        scratch_shapes=[
            VMEM((heads * seqs, LANES), jnp.float32),
            VMEM((total + SUBLANES, LANES), jnp.float32),
        ],
        compiler_params=params(16),
        name="attend",
    )(near(shares), lengths, keys, values)
    blocks = lax.all_to_all(blocks, "kv", 0, 0)
    part = pl.pallas_call(
        functools.partial(combine_kernel, seqs, heads),
        out_shape=VMEM((seqs, out_weight.shape[1]), jnp.bfloat16),
        in_specs=[vspec(), sspec(), vspec(), vspec()],
        out_specs=vspec(),
        scratch_shapes=[VMEM((heads * seqs, LANES), jnp.float32)],
        compiler_params=params(8),
        name="combine",
    )(near(blocks), lambdas, near(head_gain.reshape(1, LANES)), near(out_weight))
    if n_tp & (n_tp - 1):
        parts = list(lax.all_gather(part, "tp"))
    else:
        parts = [part] + exchanged(part, "tp", n_tp, range(1, n_tp))
    mixed = functools.reduce(jnp.add, [p.astype(jnp.float32) for p in parts])
    return mixed.astype(jnp.bfloat16)


def solution(mesh):
    in_specs = (
        P(None, "kv"),
        P("kv"),
        P("kv", "tp"),
        P(None, "kv", "tp", None),
        P(None, "kv", "tp", None),
        P(),
        P("tp"),
        P(),
        P("tp", "kv"),
    )
    step = functools.partial(body, mesh.shape["kv"], mesh.shape["tp"])
    return jax.shard_map(step, mesh=mesh, in_specs=in_specs, out_specs=P(None, "kv"), check_vma=False)
```

```python
import functools

import jax
import jax.numpy as jnp
from jax import lax
from jax.experimental import pallas as pl
from jax.experimental.pallas import tpu as pltpu
from jax.sharding import PartitionSpec as P

EPS = 1e-06
NEG = -1e30
LANES = 128
SUBLANES = 8


FLOPS, BYTES = 10**10, 10**8

VMEM = pltpu.VMEM
SMEM = pltpu.SMEM


def up(n, k):
    return -(-n // k) * k


def project_kernel(tokens_hbm, gain_hbm, weight_hbm, out_ref, tokens_ref, gain_ref, weight_ref, sems):
    copies = [
        pltpu.make_async_copy(source, target, sems.at[i])
        for i, (source, target) in enumerate(
            ((weight_hbm, weight_ref), (tokens_hbm, tokens_ref), (gain_hbm, gain_ref))
        )
    ]
    for copy in copies:
        copy.start()
    for copy in copies[::-1]:
        copy.wait()
    seqs = tokens_ref.shape[0]
    heads = weight_ref.shape[1] // LANES
    floats = tokens_ref[...].astype(jnp.float32)
    scaled = (floats * gain_ref[...]).astype(jnp.bfloat16)
    projected = jnp.dot(scaled, weight_ref[...], preferred_element_type=jnp.float32)
    squares = jnp.sum(floats * floats, axis=1, keepdims=True)
    block = [projected[:, h * LANES : (h + 1) * LANES] for h in range(heads)]
    block += [jnp.broadcast_to(squares, (seqs, LANES))]
    pad = out_ref.shape[0] - (heads + 1) * seqs
    if pad:
        block += [jnp.zeros((pad, LANES), jnp.float32)]
    out_ref[...] = jnp.concatenate(block, axis=0)


def spread_kernel(block_ref, out_ref):
    block = block_ref[...]
    for i in range(out_ref.shape[0]):
        out_ref[i] = block


def split3(x):
    high = x.astype(jnp.bfloat16).astype(jnp.float32)
    rest = x - high
    middle = rest.astype(jnp.bfloat16).astype(jnp.float32)
    return high, middle, rest - middle


def attend_kernel(width, seqs, heads, *refs):
    shares_ref, lengths_ref, keys_ref, values_ref, out_ref, query_scr, block_scr = refs
    hd = LANES // 2
    rows = 2 * heads
    columns = keys_ref.shape[1]
    span = columns // heads
    whole = jnp.sum(shares_ref[...], axis=0)
    squares = whole[heads * seqs : (heads + 1) * seqs, :]
    inverse = lax.rsqrt(squares / width + EPS) * 0.125
    for h in range(heads):
        query_scr[h * seqs : (h + 1) * seqs, :] = whole[h * seqs : (h + 1) * seqs, :] * inverse
    base = lax.axis_index("kv") * span
    lane = lax.broadcasted_iota(jnp.int32, (rows, LANES), 1)
    sub = lax.broadcasted_iota(jnp.int32, (rows, LANES), 0)
    column = lax.broadcasted_iota(jnp.int32, (rows, columns), 1)
    row = lax.broadcasted_iota(jnp.int32, (rows, columns), 0)
    mine = lax.rem(column, heads) == lax.rem(row, heads)
    peaks = jnp.zeros((rows, LANES), jnp.float32)
    masses = jnp.zeros((rows, LANES), jnp.float32)
    for s in range(seqs):
        one = query_scr[pl.ds(s, heads, stride=seqs), :]
        both = jnp.concatenate([one, one], axis=0)
        query = jnp.where((lane < hd) == (sub < heads), both, 0.0).astype(jnp.bfloat16)
        scores = lax.dot_general(
            query, keys_ref[s], (((1,), (1,)), ((), ())), preferred_element_type=jnp.float32
        )
        valid = mine & (column < (lengths_ref[s] - base) * heads)
        scores = jnp.where(valid, scores, NEG)
        peak = jnp.max(scores, axis=1, keepdims=True)
        weights = jnp.where(valid, jnp.exp(scores - peak), 0.0)
        mass = jnp.sum(weights, axis=1, keepdims=True)
        block_scr[s * rows : (s + 1) * rows, :] = jnp.dot(
            weights.astype(jnp.bfloat16), values_ref[s], preferred_element_type=jnp.float32
        )
        here = lane == s * rows + sub
        peaks = jnp.where(here, peak, peaks)
        masses = jnp.where(here, mass, masses)
    parts = split3(jnp.sum(peaks, axis=0, keepdims=True)) + split3(jnp.sum(masses, axis=0, keepdims=True))
    total = seqs * rows
    tail = lax.broadcasted_iota(jnp.int32, (SUBLANES, LANES), 0)
    stats = jnp.zeros((SUBLANES, LANES), jnp.float32)
    for i, part in enumerate(parts):
        stats = jnp.where(tail == i, part, stats)
    block_scr[total : total + SUBLANES, :] = stats
    block = block_scr[...].astype(jnp.bfloat16)
    for i in range(out_ref.shape[0]):
        out_ref[i] = block


def combine_kernel(seqs, heads, blocks_ref, lambdas_ref, gain_ref, weight_ref, out_ref, att_scr):
    shards = blocks_ref.shape[0]
    rows = 2 * heads
    total = seqs * rows
    stats = [blocks_ref[:, total + i, :].astype(jnp.float32) for i in range(6)]
    peaks = stats[0] + stats[1] + stats[2]
    masses = stats[3] + stats[4] + stats[5]
    factor = jnp.exp(peaks - jnp.max(peaks, axis=0, keepdims=True))
    mass = jnp.sum(masses * factor, axis=0, keepdims=True)
    lane = lax.broadcasted_iota(jnp.int32, (1, LANES), 1)
    sign = jnp.ones((1, LANES), jnp.float32)
    for h in range(heads):
        sign = jnp.where(lax.rem(lane, rows) == heads + h, -lambdas_ref[h], sign)
    scale = factor * (sign / mass)
    turned = jnp.transpose(scale)
    summed = jnp.zeros((total, LANES), jnp.float32)
    for k in range(shards):
        summed = summed + turned[:total, k : k + 1] * blocks_ref[k, :total, :].astype(jnp.float32)
    for s in range(seqs):
        att = summed[s * rows : s * rows + heads] + summed[s * rows + heads : (s + 1) * rows]
        norm = lax.rsqrt(jnp.mean(att * att, axis=1, keepdims=True) + EPS)
        att_scr[s * heads : (s + 1) * heads, :] = att * norm * gain_ref[...] * 0.8
    part = jnp.zeros(out_ref.shape, jnp.float32)
    for h in range(heads):
        normed = att_scr[pl.ds(h, seqs, stride=heads), :].astype(jnp.bfloat16)
        part = part + jnp.dot(
            normed, weight_ref[h * LANES : (h + 1) * LANES, :], preferred_element_type=jnp.float32
        )
    out_ref[...] = part.astype(jnp.bfloat16)


def far(x):
    return pltpu.with_memory_space_constraint(x, pltpu.HBM)


def near(x):
    return pltpu.with_memory_space_constraint(x, VMEM)


def params(limit):
    return pltpu.CompilerParams(vmem_limit_bytes=limit * 1024 * 1024)


def vspec():
    return pl.BlockSpec(memory_space=VMEM)


def hspec():
    return pl.BlockSpec(memory_space=pltpu.HBM)


def sspec():
    return pl.BlockSpec(memory_space=SMEM)


def exchanged(x, axis, n, distances):
    return [lax.ppermute(x, axis, [(i, i ^ d) for i in range(n)]) for d in distances]


def traded(x, axis, n):
    lead = 5 * n // 8
    order = [lead] + [i for i in range(n) if i != lead]
    return lax.all_to_all(x, axis, 0, 0, axis_index_groups=[order])


def body(
    n_kv,
    n_tp,
    tokens,
    norm_gain,
    query_weight,
    cache_keys,
    cache_values,
    lengths,
    lambdas,
    head_gain,
    out_weight,
):
    seqs, local = tokens.shape
    width = local * n_kv
    span, heads = cache_keys.shape[1:3]
    keys = near(cache_keys.reshape(seqs, span * heads, LANES))
    values = near(cache_values.reshape(seqs, span * heads, LANES))
    sent_rows = up((heads + 1) * seqs, SUBLANES)
    share = pl.pallas_call(
        project_kernel,
        out_shape=VMEM((sent_rows, LANES), jnp.float32),
        in_specs=[hspec(), hspec(), hspec()],
        out_specs=vspec(),
        scratch_shapes=[
            VMEM((seqs, local), tokens.dtype),
            VMEM((1, local), norm_gain.dtype),
            VMEM(query_weight.shape, query_weight.dtype),
            pltpu.SemaphoreType.DMA((3,)),
        ],
        compiler_params=params(4),
        name="project",
    )(far(tokens), far(norm_gain.reshape(1, local)), far(query_weight))
    spread = pl.pallas_call(
        spread_kernel,
        out_shape=VMEM((n_kv,) + share.shape, share.dtype),
        in_specs=[vspec()],
        out_specs=vspec(),
        compiler_params=params(4),
        cost_estimate=pl.CostEstimate(flops=FLOPS, bytes_accessed=BYTES, transcendentals=0),
        name="spread",
    )(near(share))
    shares = traded(spread, "kv", n_kv)
    total = 2 * heads * seqs
    blocks = pl.pallas_call(
        functools.partial(attend_kernel, width, seqs, heads),
        out_shape=VMEM((n_kv, total + SUBLANES, LANES), jnp.bfloat16),
        in_specs=[vspec(), sspec(), vspec(), vspec()],
        out_specs=vspec(),
        scratch_shapes=[
            VMEM((heads * seqs, LANES), jnp.float32),
            VMEM((total + SUBLANES, LANES), jnp.float32),
        ],
        compiler_params=params(16),
        name="attend",
    )(near(shares), lengths, keys, values)
    blocks = traded(blocks, "kv", n_kv)
    part = pl.pallas_call(
        functools.partial(combine_kernel, seqs, heads),
        out_shape=VMEM((seqs, out_weight.shape[1]), jnp.bfloat16),
        in_specs=[vspec(), sspec(), vspec(), vspec()],
        out_specs=vspec(),
        scratch_shapes=[VMEM((heads * seqs, LANES), jnp.float32)],
        compiler_params=params(8),
        name="combine",
    )(near(blocks), lambdas, near(head_gain.reshape(1, LANES)), near(out_weight))
    if n_tp & (n_tp - 1):
        parts = list(lax.all_gather(part, "tp"))
    else:
        parts = [part] + exchanged(part, "tp", n_tp, range(1, n_tp))
    mixed = functools.reduce(jnp.add, [p.astype(jnp.float32) for p in parts])
    return mixed.astype(jnp.bfloat16)


def solution(mesh):
    in_specs = (
        P(None, "kv"),
        P("kv"),
        P("kv", "tp"),
        P(None, "kv", "tp", None),
        P(None, "kv", "tp", None),
        P(),
        P("tp"),
        P(),
        P("tp", "kv"),
    )
    step = functools.partial(body, mesh.shape["kv"], mesh.shape["tp"])
    return jax.shard_map(step, mesh=mesh, in_specs=in_specs, out_specs=P(None, "kv"), check_vma=False)
```

```python
import functools

import jax
import jax.numpy as jnp
from jax import lax
from jax.experimental import pallas as pl
from jax.experimental.pallas import tpu as pltpu
from jax.sharding import PartitionSpec as P

EPS = 1e-06
NEG = -1e30
LANES = 128
SUBLANES = 8


FLOPS, BYTES = 10**10, 10**8

VMEM = pltpu.VMEM


def up(n, k):
    return -(-n // k) * k


def project_kernel(tokens_hbm, gain_hbm, weight_hbm, out_ref, tokens_ref, gain_ref, weight_ref, sems):
    copies = [
        pltpu.make_async_copy(source, target, sems.at[i])
        for i, (source, target) in enumerate(
            ((weight_hbm, weight_ref), (tokens_hbm, tokens_ref), (gain_hbm, gain_ref))
        )
    ]
    for copy in copies:
        copy.start()
    for copy in copies[::-1]:
        copy.wait()
    seqs = tokens_ref.shape[0]
    heads = weight_ref.shape[1] // LANES
    floats = tokens_ref[...].astype(jnp.float32)
    scaled = (floats * gain_ref[...]).astype(jnp.bfloat16)
    projected = jnp.dot(scaled, weight_ref[...], preferred_element_type=jnp.float32)
    squares = jnp.sum(floats * floats, axis=1, keepdims=True)
    block = [projected[:, h * LANES : (h + 1) * LANES] for h in range(heads)]
    block += [jnp.broadcast_to(squares, (seqs, LANES))]
    pad = out_ref.shape[0] - (heads + 1) * seqs
    if pad:
        block += [jnp.zeros((pad, LANES), jnp.float32)]
    out_ref[...] = jnp.concatenate(block, axis=0)


def spread_kernel(block_ref, out_ref):
    block = block_ref[...]
    for i in range(out_ref.shape[0]):
        out_ref[i] = block


def split3(x):
    high = x.astype(jnp.bfloat16).astype(jnp.float32)
    rest = x - high
    middle = rest.astype(jnp.bfloat16).astype(jnp.float32)
    return high, middle, rest - middle


def attend_kernel(width, seqs, heads, *refs):
    shares_ref, lengths_ref, keys_ref, values_ref, out_ref, query_scr, block_scr = refs
    hd = LANES // 2
    rows = 2 * heads
    columns = keys_ref.shape[1]
    span = columns // heads
    whole = jnp.sum(shares_ref[...], axis=0)
    squares = whole[heads * seqs : (heads + 1) * seqs, :]
    inverse = lax.rsqrt(squares / width + EPS) * 0.125
    for h in range(heads):
        query_scr[h * seqs : (h + 1) * seqs, :] = whole[h * seqs : (h + 1) * seqs, :] * inverse
    base = lax.axis_index("kv") * span
    lane = lax.broadcasted_iota(jnp.int32, (rows, LANES), 1)
    sub = lax.broadcasted_iota(jnp.int32, (rows, LANES), 0)
    column = lax.broadcasted_iota(jnp.int32, (rows, columns), 1)
    row = lax.broadcasted_iota(jnp.int32, (rows, columns), 0)
    place = jnp.where(lax.rem(column, heads) == lax.rem(row, heads), column, columns)
    scores = []
    for s in range(seqs):
        one = query_scr[pl.ds(s, heads, stride=seqs), :]
        both = jnp.concatenate([one, one], axis=0)
        query = jnp.where((lane < hd) == (sub < heads), both, 0.0).astype(jnp.bfloat16)
        scores.append(
            lax.dot_general(
                query, keys_ref[s], (((1,), (1,)), ((), ())), preferred_element_type=jnp.float32
            )
        )
    weights = []
    peaks = jnp.zeros((rows, LANES), jnp.float32)
    masses = jnp.zeros((rows, LANES), jnp.float32)
    for s in range(seqs):
        used = jnp.minimum(lengths_ref[:, s : s + 1] - base, span) * heads
        valid = place < used
        masked = jnp.where(valid, scores[s], NEG)
        peak = jnp.max(masked, axis=1, keepdims=True)
        weight = jnp.where(valid, jnp.exp(masked - peak), 0.0)
        mass = jnp.sum(weight, axis=1, keepdims=True)
        weights.append(weight.astype(jnp.bfloat16))
        here = lane == s * rows + sub
        peaks = jnp.where(here, peak, peaks)
        masses = jnp.where(here, mass, masses)
    for s in range(seqs):
        block_scr[s * rows : (s + 1) * rows, :] = jnp.dot(
            weights[s], values_ref[s], preferred_element_type=jnp.float32
        )
    parts = split3(jnp.sum(peaks, axis=0, keepdims=True)) + split3(jnp.sum(masses, axis=0, keepdims=True))
    total = seqs * rows
    tail = lax.broadcasted_iota(jnp.int32, (SUBLANES, LANES), 0)
    stats = jnp.zeros((SUBLANES, LANES), jnp.float32)
    for i, part in enumerate(parts):
        stats = jnp.where(tail == i, part, stats)
    block_scr[total : total + SUBLANES, :] = stats
    block = block_scr[...].astype(jnp.bfloat16)
    for i in range(out_ref.shape[0]):
        out_ref[i] = block


def combine_kernel(seqs, heads, blocks_ref, lambdas_ref, gain_ref, weight_ref, out_ref, att_scr):
    shards = blocks_ref.shape[0]
    rows = 2 * heads
    total = seqs * rows
    stats = [blocks_ref[:, total + i, :].astype(jnp.float32) for i in range(6)]
    peaks = stats[0] + stats[1] + stats[2]
    masses = stats[3] + stats[4] + stats[5]
    factor = jnp.exp(peaks - jnp.max(peaks, axis=0, keepdims=True))
    mass = jnp.sum(masses * factor, axis=0, keepdims=True)
    lane = lax.broadcasted_iota(jnp.int32, (1, LANES), 1)
    sign = jnp.ones((1, LANES), jnp.float32)
    for h in range(heads):
        sign = jnp.where(lax.rem(lane, rows) == heads + h, -lambdas_ref[:, h : h + 1], sign)
    scale = factor * (sign / mass)
    turned = jnp.transpose(scale)
    summed = jnp.zeros((total, LANES), jnp.float32)
    for k in range(shards):
        summed = summed + turned[:total, k : k + 1] * blocks_ref[k, :total, :].astype(jnp.float32)
    for s in range(seqs):
        att = summed[s * rows : s * rows + heads] + summed[s * rows + heads : (s + 1) * rows]
        norm = lax.rsqrt(jnp.mean(att * att, axis=1, keepdims=True) + EPS)
        att_scr[s * heads : (s + 1) * heads, :] = att * norm * gain_ref[...] * 0.8
    part = jnp.zeros(out_ref.shape, jnp.float32)
    for h in range(heads):
        normed = att_scr[pl.ds(h, seqs, stride=heads), :].astype(jnp.bfloat16)
        part = part + jnp.dot(
            normed, weight_ref[h * LANES : (h + 1) * LANES, :], preferred_element_type=jnp.float32
        )
    out_ref[...] = part.astype(jnp.bfloat16)


def far(x):
    return pltpu.with_memory_space_constraint(x, pltpu.HBM)


def near(x):
    return pltpu.with_memory_space_constraint(x, VMEM)


def params(limit):
    return pltpu.CompilerParams(vmem_limit_bytes=limit * 1024 * 1024)


def vspec():
    return pl.BlockSpec(memory_space=VMEM)


def hspec():
    return pl.BlockSpec(memory_space=pltpu.HBM)


def exchanged(x, axis, n, distances):
    return [lax.ppermute(x, axis, [(i, i ^ d) for i in range(n)]) for d in distances]


def traded(x, axis, n):
    lead = 5 * n // 8
    order = [lead] + [i for i in range(n) if i != lead]
    return lax.all_to_all(x, axis, 0, 0, axis_index_groups=[order])


def body(
    n_kv,
    n_tp,
    tokens,
    norm_gain,
    query_weight,
    cache_keys,
    cache_values,
    lengths,
    lambdas,
    head_gain,
    out_weight,
):
    seqs, local = tokens.shape
    width = local * n_kv
    span, heads = cache_keys.shape[1:3]
    keys = near(cache_keys.reshape(seqs, span * heads, LANES))
    values = near(cache_values.reshape(seqs, span * heads, LANES))
    sent_rows = up((heads + 1) * seqs, SUBLANES)
    share = pl.pallas_call(
        project_kernel,
        out_shape=VMEM((sent_rows, LANES), jnp.float32),
        in_specs=[hspec(), hspec(), hspec()],
        out_specs=vspec(),
        scratch_shapes=[
            VMEM((seqs, local), tokens.dtype),
            VMEM((1, local), norm_gain.dtype),
            VMEM(query_weight.shape, query_weight.dtype),
            pltpu.SemaphoreType.DMA((3,)),
        ],
        compiler_params=params(4),
        name="project",
    )(far(tokens), far(norm_gain.reshape(1, local)), far(query_weight))
    spread = pl.pallas_call(
        spread_kernel,
        out_shape=VMEM((n_kv,) + share.shape, share.dtype),
        in_specs=[vspec()],
        out_specs=vspec(),
        compiler_params=params(4),
        cost_estimate=pl.CostEstimate(flops=FLOPS, bytes_accessed=BYTES, transcendentals=0),
        name="spread",
    )(near(share))
    shares = traded(spread, "kv", n_kv)
    total = 2 * heads * seqs
    blocks = pl.pallas_call(
        functools.partial(attend_kernel, width, seqs, heads),
        out_shape=VMEM((n_kv, total + SUBLANES, LANES), jnp.bfloat16),
        in_specs=[vspec()] * 4,
        out_specs=vspec(),
        scratch_shapes=[
            VMEM((heads * seqs, LANES), jnp.float32),
            VMEM((total + SUBLANES, LANES), jnp.float32),
        ],
        compiler_params=params(16),
        name="attend",
    )(near(shares), near(lengths.reshape(1, seqs)), keys, values)
    blocks = traded(blocks, "kv", n_kv)
    part = pl.pallas_call(
        functools.partial(combine_kernel, seqs, heads),
        out_shape=VMEM((seqs, out_weight.shape[1]), jnp.bfloat16),
        in_specs=[vspec()] * 4,
        out_specs=vspec(),
        scratch_shapes=[VMEM((heads * seqs, LANES), jnp.float32)],
        compiler_params=params(8),
        name="combine",
    )(near(blocks), near(lambdas.reshape(1, heads)), near(head_gain.reshape(1, LANES)), near(out_weight))
    if n_tp & (n_tp - 1):
        parts = list(lax.all_gather(part, "tp"))
    else:
        parts = [part] + exchanged(part, "tp", n_tp, range(1, n_tp))
    mixed = functools.reduce(jnp.add, [p.astype(jnp.float32) for p in parts])
    return mixed.astype(jnp.bfloat16)


def solution(mesh):
    in_specs = (
        P(None, "kv"),
        P("kv"),
        P("kv", "tp"),
        P(None, "kv", "tp", None),
        P(None, "kv", "tp", None),
        P(),
        P("tp"),
        P(),
        P("tp", "kv"),
    )
    step = functools.partial(body, mesh.shape["kv"], mesh.shape["tp"])
    return jax.shard_map(step, mesh=mesh, in_specs=in_specs, out_specs=P(None, "kv"), check_vma=False)
```

```python
import functools

import jax
import jax.numpy as jnp
from jax import lax
from jax.experimental import pallas as pl
from jax.experimental.pallas import tpu as pltpu
from jax.sharding import PartitionSpec as P

EPS = 1e-06
NEG = -1e30
LANES = 128
SUBLANES = 8


FLOPS, BYTES = 10**10, 10**8

VMEM = pltpu.VMEM


def project_kernel(tokens_hbm, gain_hbm, weight_hbm, out_ref, tokens_ref, gain_ref, weight_ref, sems):
    copies = [
        pltpu.make_async_copy(source, target, sems.at[i])
        for i, (source, target) in enumerate(
            ((weight_hbm, weight_ref), (tokens_hbm, tokens_ref), (gain_hbm, gain_ref))
        )
    ]
    for copy in copies:
        copy.start()
    for copy in copies[::-1]:
        copy.wait()
    seqs = tokens_ref.shape[0]
    heads = weight_ref.shape[1] // LANES
    floats = tokens_ref[...].astype(jnp.float32)
    scaled = (floats * gain_ref[...]).astype(jnp.bfloat16)
    projected = jnp.dot(scaled, weight_ref[...], preferred_element_type=jnp.float32)
    for h in range(heads):
        out_ref[h] = projected[:, h * LANES : (h + 1) * LANES]
    squares = jnp.sum(floats * floats, axis=1, keepdims=True)
    out_ref[heads] = jnp.broadcast_to(squares, (seqs, LANES))


def spread_kernel(block_ref, out_ref):
    block = block_ref[...]
    for i in range(out_ref.shape[0]):
        out_ref[i] = block


def split3(x):
    high = x.astype(jnp.bfloat16).astype(jnp.float32)
    rest = x - high
    middle = rest.astype(jnp.bfloat16).astype(jnp.float32)
    return high, middle, rest - middle


def attend_kernel(width, seqs, heads, *refs):
    shares_ref, lengths_ref, keys_ref, values_ref, out_ref, query_scr, block_scr = refs
    hd = LANES // 2
    rows = 2 * heads
    columns = keys_ref.shape[1]
    span = columns // heads
    whole = jnp.sum(shares_ref[...], axis=0)
    inverse = lax.rsqrt(whole[heads] / width + EPS) * 0.125
    for h in range(heads):
        query_scr[h * seqs : (h + 1) * seqs, :] = whole[h] * inverse
    base = lax.axis_index("kv") * span
    lane = lax.broadcasted_iota(jnp.int32, (rows, LANES), 1)
    sub = lax.broadcasted_iota(jnp.int32, (rows, LANES), 0)
    column = lax.broadcasted_iota(jnp.int32, (rows, columns), 1)
    row = lax.broadcasted_iota(jnp.int32, (rows, columns), 0)
    slot = lax.div(sub, heads) * heads * seqs + lax.rem(sub, heads) * seqs
    place = jnp.where(lax.rem(column, heads) == lax.rem(row, heads), column, columns)
    scores = []
    for s in range(seqs):
        one = query_scr[pl.ds(s, heads, stride=seqs), :]
        both = jnp.concatenate([one, one], axis=0)
        query = jnp.where((lane < hd) == (sub < heads), both, 0.0).astype(jnp.bfloat16)
        scores.append(
            lax.dot_general(
                query, keys_ref[s], (((1,), (1,)), ((), ())), preferred_element_type=jnp.float32
            )
        )
    weights = []
    peaks = jnp.zeros((rows, LANES), jnp.float32)
    masses = jnp.zeros((rows, LANES), jnp.float32)
    for s in range(seqs):
        used = jnp.minimum(lengths_ref[:, s : s + 1] - base, span) * heads
        valid = place < used
        masked = jnp.where(valid, scores[s], NEG)
        peak = jnp.max(masked, axis=1, keepdims=True)
        weight = jnp.where(valid, jnp.exp(masked - peak), 0.0)
        mass = jnp.sum(weight, axis=1, keepdims=True)
        weights.append(weight.astype(jnp.bfloat16))
        here = lane == slot + s
        peaks = jnp.where(here, peak, peaks)
        masses = jnp.where(here, mass, masses)
    for s in range(seqs):
        summed = jnp.dot(weights[s], values_ref[s], preferred_element_type=jnp.float32)
        for m in range(2):
            block_scr[pl.ds(m * heads * seqs + s, heads, stride=seqs), :] = summed[m * heads : (m + 1) * heads]
    parts = split3(jnp.sum(peaks, axis=0, keepdims=True)) + split3(jnp.sum(masses, axis=0, keepdims=True))
    total = seqs * rows
    tail = lax.broadcasted_iota(jnp.int32, (SUBLANES, LANES), 0)
    stats = jnp.zeros((SUBLANES, LANES), jnp.float32)
    for i, part in enumerate(parts):
        stats = jnp.where(tail == i, part, stats)
    block_scr[total : total + SUBLANES, :] = stats
    block = block_scr[...].astype(jnp.bfloat16)
    for i in range(out_ref.shape[0]):
        out_ref[i] = block


def combine_kernel(seqs, heads, blocks_ref, lambdas_ref, gain_ref, weight_ref, out_ref):
    shards = blocks_ref.shape[0]
    half = heads * seqs
    total = 2 * half
    stats = [blocks_ref[:, total + i, :].astype(jnp.float32) for i in range(6)]
    peaks = stats[0] + stats[1] + stats[2]
    masses = stats[3] + stats[4] + stats[5]
    factor = jnp.exp(peaks - jnp.max(peaks, axis=0, keepdims=True))
    mass = jnp.sum(masses * factor, axis=0, keepdims=True)
    lane = lax.broadcasted_iota(jnp.int32, (1, LANES), 1)
    sign = jnp.ones((1, LANES), jnp.float32)
    for h in range(heads):
        sign = jnp.where(lax.div(lane, seqs) == heads + h, -lambdas_ref[:, h : h + 1], sign)
    turned = jnp.transpose(factor * (sign / mass))
    summed = jnp.zeros((total, LANES), jnp.float32)
    for k in range(shards):
        summed = summed + turned[:total, k : k + 1] * blocks_ref[k, :total, :].astype(jnp.float32)
    attended = summed[:half] + summed[half:]
    norm = lax.rsqrt(jnp.mean(attended * attended, axis=1, keepdims=True) + EPS) * 0.8
    gained = (attended * gain_ref[...]).astype(jnp.bfloat16)
    part = jnp.zeros(out_ref.shape, jnp.float32)
    for h in range(heads):
        rows = slice(h * seqs, (h + 1) * seqs)
        part = part + norm[rows] * jnp.dot(
            gained[rows], weight_ref[h * LANES : (h + 1) * LANES, :], preferred_element_type=jnp.float32
        )
    out_ref[...] = part.astype(jnp.bfloat16)


def far(x):
    return pltpu.with_memory_space_constraint(x, pltpu.HBM)


def near(x):
    return pltpu.with_memory_space_constraint(x, VMEM)


def params(limit):
    return pltpu.CompilerParams(vmem_limit_bytes=limit * 1024 * 1024)


def vspec():
    return pl.BlockSpec(memory_space=VMEM)


def hspec():
    return pl.BlockSpec(memory_space=pltpu.HBM)


def exchanged(x, axis, n, distances):
    return [lax.ppermute(x, axis, [(i, i ^ d) for i in range(n)]) for d in distances]


def traded(x, axis, n):
    lead = 5 * n // 8
    order = [lead] + [i for i in range(n) if i != lead]
    return lax.all_to_all(x, axis, 0, 0, axis_index_groups=[order])


def body(
    n_kv,
    n_tp,
    tokens,
    norm_gain,
    query_weight,
    cache_keys,
    cache_values,
    lengths,
    lambdas,
    head_gain,
    out_weight,
):
    seqs, local = tokens.shape
    width = local * n_kv
    span, heads = cache_keys.shape[1:3]
    keys = near(cache_keys.reshape(seqs, span * heads, LANES))
    values = near(cache_values.reshape(seqs, span * heads, LANES))
    share = pl.pallas_call(
        project_kernel,
        out_shape=VMEM((heads + 1, seqs, LANES), jnp.float32),
        in_specs=[hspec(), hspec(), hspec()],
        out_specs=vspec(),
        scratch_shapes=[
            VMEM((seqs, local), tokens.dtype),
            VMEM((1, local), norm_gain.dtype),
            VMEM(query_weight.shape, query_weight.dtype),
            pltpu.SemaphoreType.DMA((3,)),
        ],
        compiler_params=params(4),
        name="project",
    )(far(tokens), far(norm_gain.reshape(1, local)), far(query_weight))
    spread = pl.pallas_call(
        spread_kernel,
        out_shape=VMEM((n_kv,) + share.shape, share.dtype),
        in_specs=[vspec()],
        out_specs=vspec(),
        compiler_params=params(4),
        cost_estimate=pl.CostEstimate(flops=FLOPS, bytes_accessed=BYTES, transcendentals=0),
        name="spread",
    )(near(share))
    shares = traded(spread, "kv", n_kv)
    total = 2 * heads * seqs
    blocks = pl.pallas_call(
        functools.partial(attend_kernel, width, seqs, heads),
        out_shape=VMEM((n_kv, total + SUBLANES, LANES), jnp.bfloat16),
        in_specs=[vspec()] * 4,
        out_specs=vspec(),
        scratch_shapes=[
            VMEM((heads * seqs, LANES), jnp.float32),
            VMEM((total + SUBLANES, LANES), jnp.float32),
        ],
        compiler_params=params(16),
        name="attend",
    )(near(shares), near(lengths.reshape(1, seqs)), keys, values)
    blocks = traded(blocks, "kv", n_kv)
    part = pl.pallas_call(
        functools.partial(combine_kernel, seqs, heads),
        out_shape=VMEM((seqs, out_weight.shape[1]), jnp.bfloat16),
        in_specs=[vspec()] * 4,
        out_specs=vspec(),
        compiler_params=params(8),
        name="combine",
    )(near(blocks), near(lambdas.reshape(1, heads)), near(head_gain.reshape(1, LANES)), near(out_weight))
    if n_tp & (n_tp - 1):
        parts = list(lax.all_gather(part, "tp"))
    else:
        parts = [part] + exchanged(part, "tp", n_tp, range(1, n_tp))
    mixed = functools.reduce(jnp.add, [p.astype(jnp.float32) for p in parts])
    return mixed.astype(jnp.bfloat16)


def solution(mesh):
    in_specs = (
        P(None, "kv"),
        P("kv"),
        P("kv", "tp"),
        P(None, "kv", "tp", None),
        P(None, "kv", "tp", None),
        P(),
        P("tp"),
        P(),
        P("tp", "kv"),
    )
    step = functools.partial(body, mesh.shape["kv"], mesh.shape["tp"])
    return jax.shard_map(step, mesh=mesh, in_specs=in_specs, out_specs=P(None, "kv"), check_vma=False)
```

```python
import functools

import jax
import jax.numpy as jnp
from jax import lax
from jax.experimental import pallas as pl
from jax.experimental.pallas import tpu as pltpu
from jax.sharding import PartitionSpec as P

EPS = 1e-06
NEG = -1e30
LANES = 128
SUBLANES = 8


FLOPS, BYTES = 10**10, 10**8

VMEM = pltpu.VMEM


def project_kernel(tokens_hbm, gain_hbm, weight_hbm, out_ref, tokens_ref, gain_ref, weight_ref, sems):
    copies = [
        pltpu.make_async_copy(source, target, sems.at[i])
        for i, (source, target) in enumerate(
            ((weight_hbm, weight_ref), (tokens_hbm, tokens_ref), (gain_hbm, gain_ref))
        )
    ]
    for copy in copies:
        copy.start()
    for copy in copies[::-1]:
        copy.wait()
    seqs = tokens_ref.shape[0]
    heads = weight_ref.shape[1] // LANES
    floats = tokens_ref[...].astype(jnp.float32)
    scaled = (floats * gain_ref[...]).astype(jnp.bfloat16)
    projected = jnp.dot(scaled, weight_ref[...], preferred_element_type=jnp.float32)
    squares = jnp.broadcast_to(jnp.sum(floats * floats, axis=1, keepdims=True), (seqs, LANES))
    for i in range(out_ref.shape[0]):
        for h in range(heads):
            out_ref[i, h] = projected[:, h * LANES : (h + 1) * LANES]
        out_ref[i, heads] = squares


def split3(x):
    high = x.astype(jnp.bfloat16).astype(jnp.float32)
    rest = x - high
    middle = rest.astype(jnp.bfloat16).astype(jnp.float32)
    return high, middle, rest - middle


def attend_kernel(width, seqs, heads, *refs):
    shares_ref, lengths_ref, keys_ref, values_ref, out_ref, query_scr, block_scr = refs
    hd = LANES // 2
    rows = 2 * heads
    columns = keys_ref.shape[1]
    span = columns // heads
    whole = jnp.sum(shares_ref[...], axis=0)
    inverse = lax.rsqrt(whole[heads] / width + EPS) * 0.125
    for h in range(heads):
        query_scr[h * seqs : (h + 1) * seqs, :] = whole[h] * inverse
    base = lax.axis_index("kv") * span
    lane = lax.broadcasted_iota(jnp.int32, (rows, LANES), 1)
    sub = lax.broadcasted_iota(jnp.int32, (rows, LANES), 0)
    column = lax.broadcasted_iota(jnp.int32, (rows, columns), 1)
    row = lax.broadcasted_iota(jnp.int32, (rows, columns), 0)
    slot = lax.div(sub, heads) * heads * seqs + lax.rem(sub, heads) * seqs
    place = jnp.where(lax.rem(column, heads) == lax.rem(row, heads), column, columns)
    scores = []
    for s in range(seqs):
        one = query_scr[pl.ds(s, heads, stride=seqs), :]
        both = jnp.concatenate([one, one], axis=0)
        query = jnp.where((lane < hd) == (sub < heads), both, 0.0).astype(jnp.bfloat16)
        scores.append(
            lax.dot_general(
                query, keys_ref[s], (((1,), (1,)), ((), ())), preferred_element_type=jnp.float32
            )
        )
    weights = []
    peaks = jnp.zeros((rows, LANES), jnp.float32)
    masses = jnp.zeros((rows, LANES), jnp.float32)
    for s in range(seqs):
        used = jnp.minimum(lengths_ref[:, s : s + 1] - base, span) * heads
        valid = place < used
        masked = jnp.where(valid, scores[s], NEG)
        peak = jnp.max(masked, axis=1, keepdims=True)
        weight = jnp.where(valid, jnp.exp(masked - peak), 0.0)
        mass = jnp.sum(weight, axis=1, keepdims=True)
        weights.append(weight.astype(jnp.bfloat16))
        here = lane == slot + s
        peaks = jnp.where(here, peak, peaks)
        masses = jnp.where(here, mass, masses)
    for s in range(seqs):
        summed = jnp.dot(weights[s], values_ref[s], preferred_element_type=jnp.float32)
        for m in range(2):
            block_scr[pl.ds(m * heads * seqs + s, heads, stride=seqs), :] = summed[m * heads : (m + 1) * heads]
    parts = split3(jnp.sum(peaks, axis=0, keepdims=True)) + split3(jnp.sum(masses, axis=0, keepdims=True))
    total = seqs * rows
    tail = lax.broadcasted_iota(jnp.int32, (SUBLANES, LANES), 0)
    stats = jnp.zeros((SUBLANES, LANES), jnp.float32)
    for i, part in enumerate(parts):
        stats = jnp.where(tail == i, part, stats)
    block_scr[total : total + SUBLANES, :] = stats
    block = block_scr[...].astype(jnp.bfloat16)
    for i in range(out_ref.shape[0]):
        out_ref[i] = block


def combine_kernel(seqs, heads, blocks_ref, lambdas_ref, gain_ref, weight_ref, out_ref):
    shards = blocks_ref.shape[0]
    half = heads * seqs
    total = 2 * half
    stats = [blocks_ref[:, total + i, :].astype(jnp.float32) for i in range(6)]
    peaks = stats[0] + stats[1] + stats[2]
    masses = stats[3] + stats[4] + stats[5]
    factor = jnp.exp(peaks - jnp.max(peaks, axis=0, keepdims=True))
    mass = jnp.sum(masses * factor, axis=0, keepdims=True)
    lane = lax.broadcasted_iota(jnp.int32, (1, LANES), 1)
    sign = jnp.ones((1, LANES), jnp.float32)
    for h in range(heads):
        sign = jnp.where(lax.div(lane, seqs) == heads + h, -lambdas_ref[:, h : h + 1], sign)
    turned = jnp.transpose(factor * (sign / mass))
    summed = jnp.zeros((total, LANES), jnp.float32)
    for k in range(shards):
        summed = summed + turned[:total, k : k + 1] * blocks_ref[k, :total, :].astype(jnp.float32)
    attended = summed[:half] + summed[half:]
    norm = lax.rsqrt(jnp.mean(attended * attended, axis=1, keepdims=True) + EPS) * 0.8
    gained = (attended * gain_ref[...]).astype(jnp.bfloat16)
    part = jnp.zeros(out_ref.shape, jnp.float32)
    for h in range(heads):
        rows = slice(h * seqs, (h + 1) * seqs)
        part = part + norm[rows] * jnp.dot(
            gained[rows], weight_ref[h * LANES : (h + 1) * LANES, :], preferred_element_type=jnp.float32
        )
    out_ref[...] = part.astype(jnp.bfloat16)


def far(x):
    return pltpu.with_memory_space_constraint(x, pltpu.HBM)


def near(x):
    return pltpu.with_memory_space_constraint(x, VMEM)


def params(limit):
    return pltpu.CompilerParams(vmem_limit_bytes=limit * 1024 * 1024)


def vspec():
    return pl.BlockSpec(memory_space=VMEM)


def hspec():
    return pl.BlockSpec(memory_space=pltpu.HBM)


def exchanged(x, axis, n, distances):
    return [lax.ppermute(x, axis, [(i, i ^ d) for i in range(n)]) for d in distances]


def traded(x, axis, n):
    lead = 5 * n // 8
    order = [lead] + [i for i in range(n) if i != lead]
    return lax.all_to_all(x, axis, 0, 0, axis_index_groups=[order])


def body(
    n_kv,
    n_tp,
    tokens,
    norm_gain,
    query_weight,
    cache_keys,
    cache_values,
    lengths,
    lambdas,
    head_gain,
    out_weight,
):
    seqs, local = tokens.shape
    width = local * n_kv
    span, heads = cache_keys.shape[1:3]
    keys = near(cache_keys.reshape(seqs, span * heads, LANES))
    values = near(cache_values.reshape(seqs, span * heads, LANES))
    share = pl.pallas_call(
        project_kernel,
        out_shape=VMEM((n_kv, heads + 1, seqs, LANES), jnp.float32),
        in_specs=[hspec(), hspec(), hspec()],
        out_specs=vspec(),
        scratch_shapes=[
            VMEM((seqs, local), tokens.dtype),
            VMEM((1, local), norm_gain.dtype),
            VMEM(query_weight.shape, query_weight.dtype),
            pltpu.SemaphoreType.DMA((3,)),
        ],
        compiler_params=params(4),
        cost_estimate=pl.CostEstimate(flops=FLOPS, bytes_accessed=BYTES, transcendentals=0),
        name="project",
    )(far(tokens), far(norm_gain.reshape(1, local)), far(query_weight))
    shares = traded(share, "kv", n_kv)
    total = 2 * heads * seqs
    blocks = pl.pallas_call(
        functools.partial(attend_kernel, width, seqs, heads),
        out_shape=VMEM((n_kv, total + SUBLANES, LANES), jnp.bfloat16),
        in_specs=[vspec()] * 4,
        out_specs=vspec(),
        scratch_shapes=[
            VMEM((heads * seqs, LANES), jnp.float32),
            VMEM((total + SUBLANES, LANES), jnp.float32),
        ],
        compiler_params=params(16),
        name="attend",
    )(near(shares), near(lengths.reshape(1, seqs)), keys, values)
    blocks = traded(blocks, "kv", n_kv)
    part = pl.pallas_call(
        functools.partial(combine_kernel, seqs, heads),
        out_shape=VMEM((seqs, out_weight.shape[1]), jnp.bfloat16),
        in_specs=[vspec()] * 4,
        out_specs=vspec(),
        compiler_params=params(8),
        name="combine",
    )(near(blocks), near(lambdas.reshape(1, heads)), near(head_gain.reshape(1, LANES)), near(out_weight))
    if n_tp & (n_tp - 1):
        parts = list(lax.all_gather(part, "tp"))
    else:
        parts = [part] + exchanged(part, "tp", n_tp, range(1, n_tp))
    mixed = functools.reduce(jnp.add, [p.astype(jnp.float32) for p in parts])
    return mixed.astype(jnp.bfloat16)


def solution(mesh):
    in_specs = (
        P(None, "kv"),
        P("kv"),
        P("kv", "tp"),
        P(None, "kv", "tp", None),
        P(None, "kv", "tp", None),
        P(),
        P("tp"),
        P(),
        P("tp", "kv"),
    )
    step = functools.partial(body, mesh.shape["kv"], mesh.shape["tp"])
    return jax.shard_map(step, mesh=mesh, in_specs=in_specs, out_specs=P(None, "kv"), check_vma=False)
```

```python
import functools

import jax
import jax.numpy as jnp
from jax import lax
from jax.experimental import pallas as pl
from jax.experimental.pallas import tpu as pltpu
from jax.sharding import PartitionSpec as P

EPS = 1e-06
NEG = -1e30
LANES = 128
SUBLANES = 8


FLOPS, BYTES = 10**10, 10**8

ORDER = (5, 4, 1, 0, 6, 7, 2, 3)

VMEM = pltpu.VMEM


def project_kernel(tokens_hbm, gain_hbm, weight_hbm, out_ref, tokens_ref, gain_ref, weight_ref, sems):
    copies = [
        pltpu.make_async_copy(source, target, sems.at[i])
        for i, (source, target) in enumerate(
            ((weight_hbm, weight_ref), (tokens_hbm, tokens_ref), (gain_hbm, gain_ref))
        )
    ]
    for copy in copies:
        copy.start()
    for copy in copies[::-1]:
        copy.wait()
    seqs = tokens_ref.shape[0]
    heads = weight_ref.shape[1] // LANES
    floats = tokens_ref[...].astype(jnp.float32)
    scaled = (floats * gain_ref[...]).astype(jnp.bfloat16)
    projected = jnp.dot(scaled, weight_ref[...], preferred_element_type=jnp.float32)
    squares = jnp.broadcast_to(jnp.sum(floats * floats, axis=1, keepdims=True), (seqs, LANES))
    for i in range(out_ref.shape[0]):
        for h in range(heads):
            out_ref[i, h] = projected[:, h * LANES : (h + 1) * LANES]
        out_ref[i, heads] = squares


def split3(x):
    high = x.astype(jnp.bfloat16).astype(jnp.float32)
    rest = x - high
    middle = rest.astype(jnp.bfloat16).astype(jnp.float32)
    return high, middle, rest - middle


def attend_kernel(width, seqs, heads, *refs):
    shares_ref, lengths_ref, keys_ref, values_ref, out_ref, query_scr, block_scr = refs
    hd = LANES // 2
    rows = 2 * heads
    columns = keys_ref.shape[1]
    span = columns // heads
    whole = jnp.sum(shares_ref[...], axis=0)
    inverse = lax.rsqrt(whole[heads] / width + EPS) * 0.125
    for h in range(heads):
        query_scr[h * seqs : (h + 1) * seqs, :] = whole[h] * inverse
    base = lax.axis_index("kv") * span
    lane = lax.broadcasted_iota(jnp.int32, (rows, LANES), 1)
    sub = lax.broadcasted_iota(jnp.int32, (rows, LANES), 0)
    column = lax.broadcasted_iota(jnp.int32, (rows, columns), 1)
    row = lax.broadcasted_iota(jnp.int32, (rows, columns), 0)
    slot = lax.div(sub, heads) * heads * seqs + lax.rem(sub, heads) * seqs
    place = jnp.where(lax.rem(column, heads) == lax.rem(row, heads), column, columns)
    scores = []
    for s in range(seqs):
        one = query_scr[pl.ds(s, heads, stride=seqs), :]
        both = jnp.concatenate([one, one], axis=0)
        query = jnp.where((lane < hd) == (sub < heads), both, 0.0).astype(jnp.bfloat16)
        scores.append(
            lax.dot_general(
                query, keys_ref[s], (((1,), (1,)), ((), ())), preferred_element_type=jnp.float32
            )
        )
    weights = []
    peaks = jnp.zeros((rows, LANES), jnp.float32)
    masses = jnp.zeros((rows, LANES), jnp.float32)
    for s in range(seqs):
        used = jnp.minimum(lengths_ref[:, s : s + 1] - base, span) * heads
        valid = place < used
        masked = jnp.where(valid, scores[s], NEG)
        peak = jnp.max(masked, axis=1, keepdims=True)
        weight = jnp.where(valid, jnp.exp(masked - peak), 0.0)
        mass = jnp.sum(weight, axis=1, keepdims=True)
        weights.append(weight.astype(jnp.bfloat16))
        here = lane == slot + s
        peaks = jnp.where(here, peak, peaks)
        masses = jnp.where(here, mass, masses)
    for s in range(seqs):
        summed = jnp.dot(weights[s], values_ref[s], preferred_element_type=jnp.float32)
        for m in range(2):
            block_scr[pl.ds(m * heads * seqs + s, heads, stride=seqs), :] = summed[m * heads : (m + 1) * heads]
    parts = split3(jnp.sum(peaks, axis=0, keepdims=True)) + split3(jnp.sum(masses, axis=0, keepdims=True))
    total = seqs * rows
    tail = lax.broadcasted_iota(jnp.int32, (SUBLANES, LANES), 0)
    stats = jnp.zeros((SUBLANES, LANES), jnp.float32)
    for i, part in enumerate(parts):
        stats = jnp.where(tail == i, part, stats)
    block_scr[total : total + SUBLANES, :] = stats
    block = block_scr[...].astype(jnp.bfloat16)
    for i in range(out_ref.shape[0]):
        out_ref[i] = block


def combine_kernel(seqs, heads, blocks_ref, lambdas_ref, gain_ref, weight_ref, out_ref):
    shards = blocks_ref.shape[0]
    half = heads * seqs
    total = 2 * half
    stats = [blocks_ref[:, total + i, :].astype(jnp.float32) for i in range(6)]
    peaks = stats[0] + stats[1] + stats[2]
    masses = stats[3] + stats[4] + stats[5]
    factor = jnp.exp(peaks - jnp.max(peaks, axis=0, keepdims=True))
    mass = jnp.sum(masses * factor, axis=0, keepdims=True)
    lane = lax.broadcasted_iota(jnp.int32, (1, LANES), 1)
    sign = jnp.ones((1, LANES), jnp.float32)
    for h in range(heads):
        sign = jnp.where(lax.div(lane, seqs) == heads + h, -lambdas_ref[:, h : h + 1], sign)
    turned = jnp.transpose(factor * (sign / mass))
    summed = jnp.zeros((total, LANES), jnp.float32)
    for k in range(shards):
        summed = summed + turned[:total, k : k + 1] * blocks_ref[k, :total, :].astype(jnp.float32)
    attended = summed[:half] + summed[half:]
    norm = lax.rsqrt(jnp.mean(attended * attended, axis=1, keepdims=True) + EPS) * 0.8
    gained = (attended * gain_ref[...]).astype(jnp.bfloat16)
    part = jnp.zeros(out_ref.shape, jnp.float32)
    for h in range(heads):
        rows = slice(h * seqs, (h + 1) * seqs)
        part = part + norm[rows] * jnp.dot(
            gained[rows], weight_ref[h * LANES : (h + 1) * LANES, :], preferred_element_type=jnp.float32
        )
    out_ref[...] = part.astype(jnp.bfloat16)


def far(x):
    return pltpu.with_memory_space_constraint(x, pltpu.HBM)


def near(x):
    return pltpu.with_memory_space_constraint(x, VMEM)


def params(limit):
    return pltpu.CompilerParams(vmem_limit_bytes=limit * 1024 * 1024)


def vspec():
    return pl.BlockSpec(memory_space=VMEM)


def hspec():
    return pl.BlockSpec(memory_space=pltpu.HBM)


def exchanged(x, axis, n, distances):
    return [lax.ppermute(x, axis, [(i, i ^ d) for i in range(n)]) for d in distances]


def traded(x, axis, n):
    parts = len(ORDER)
    if n % parts:
        order = sorted(range(n), key=lambda i: i != 5 * n // 8)
    else:
        order = [part * (n // parts) + i for part in ORDER for i in range(n // parts)]
    return lax.all_to_all(x, axis, 0, 0, axis_index_groups=[order])


def body(
    n_kv,
    n_tp,
    tokens,
    norm_gain,
    query_weight,
    cache_keys,
    cache_values,
    lengths,
    lambdas,
    head_gain,
    out_weight,
):
    seqs, local = tokens.shape
    width = local * n_kv
    span, heads = cache_keys.shape[1:3]
    keys = near(cache_keys.reshape(seqs, span * heads, LANES))
    values = near(cache_values.reshape(seqs, span * heads, LANES))
    share = pl.pallas_call(
        project_kernel,
        out_shape=VMEM((n_kv, heads + 1, seqs, LANES), jnp.float32),
        in_specs=[hspec(), hspec(), hspec()],
        out_specs=vspec(),
        scratch_shapes=[
            VMEM((seqs, local), tokens.dtype),
            VMEM((1, local), norm_gain.dtype),
            VMEM(query_weight.shape, query_weight.dtype),
            pltpu.SemaphoreType.DMA((3,)),
        ],
        compiler_params=params(4),
        cost_estimate=pl.CostEstimate(flops=FLOPS, bytes_accessed=BYTES, transcendentals=0),
        name="project",
    )(far(tokens), far(norm_gain.reshape(1, local)), far(query_weight))
    shares = traded(share, "kv", n_kv)
    total = 2 * heads * seqs
    blocks = pl.pallas_call(
        functools.partial(attend_kernel, width, seqs, heads),
        out_shape=VMEM((n_kv, total + SUBLANES, LANES), jnp.bfloat16),
        in_specs=[vspec()] * 4,
        out_specs=vspec(),
        scratch_shapes=[
            VMEM((heads * seqs, LANES), jnp.float32),
            VMEM((total + SUBLANES, LANES), jnp.float32),
        ],
        compiler_params=params(16),
        name="attend",
    )(near(shares), near(lengths.reshape(1, seqs)), keys, values)
    blocks = traded(blocks, "kv", n_kv)
    part = pl.pallas_call(
        functools.partial(combine_kernel, seqs, heads),
        out_shape=VMEM((seqs, out_weight.shape[1]), jnp.bfloat16),
        in_specs=[vspec()] * 4,
        out_specs=vspec(),
        compiler_params=params(8),
        name="combine",
    )(near(blocks), near(lambdas.reshape(1, heads)), near(head_gain.reshape(1, LANES)), near(out_weight))
    if n_tp & (n_tp - 1):
        parts = list(lax.all_gather(part, "tp"))
    else:
        parts = [part] + exchanged(part, "tp", n_tp, range(1, n_tp))
    mixed = functools.reduce(jnp.add, [p.astype(jnp.float32) for p in parts])
    return mixed.astype(jnp.bfloat16)


def solution(mesh):
    in_specs = (
        P(None, "kv"),
        P("kv"),
        P("kv", "tp"),
        P(None, "kv", "tp", None),
        P(None, "kv", "tp", None),
        P(),
        P("tp"),
        P(),
        P("tp", "kv"),
    )
    step = functools.partial(body, mesh.shape["kv"], mesh.shape["tp"])
    return jax.shard_map(step, mesh=mesh, in_specs=in_specs, out_specs=P(None, "kv"), check_vma=False)
```

```python
import functools

import jax
import jax.numpy as jnp
from jax import lax
from jax.experimental import pallas as pl
from jax.experimental.pallas import tpu as pltpu
from jax.sharding import PartitionSpec as P

EPS = 1e-06
NEG = -1e30
LANES = 128
SUBLANES = 8


FLOPS, BYTES = 10**10, 10**8

ORDER = (5, 4, 1, 0, 6, 7, 2, 3)

VMEM = pltpu.VMEM


def project_kernel(tokens_hbm, gain_hbm, weight_hbm, out_ref, tokens_ref, gain_ref, weight_ref, sems):
    copies = [
        pltpu.make_async_copy(source, target, sems.at[i])
        for i, (source, target) in enumerate(
            ((tokens_hbm, tokens_ref), (gain_hbm, gain_ref), (weight_hbm, weight_ref))
        )
    ]
    for copy in copies:
        copy.start()
    for copy in copies:
        copy.wait()
    seqs = tokens_ref.shape[0]
    heads = weight_ref.shape[1] // LANES
    floats = tokens_ref[...].astype(jnp.float32)
    scaled = (floats * gain_ref[...]).astype(jnp.bfloat16)
    projected = jnp.dot(scaled, weight_ref[...], preferred_element_type=jnp.float32)
    squares = jnp.broadcast_to(jnp.sum(floats * floats, axis=1, keepdims=True), (seqs, LANES))
    for i in range(out_ref.shape[0]):
        for h in range(heads):
            out_ref[i, h] = projected[:, h * LANES : (h + 1) * LANES]
        out_ref[i, heads] = squares


def split3(x):
    high = x.astype(jnp.bfloat16).astype(jnp.float32)
    rest = x - high
    middle = rest.astype(jnp.bfloat16).astype(jnp.float32)
    return high, middle, rest - middle


def attend_kernel(width, seqs, heads, *refs):
    shares_ref, lengths_ref, keys_ref, values_ref, out_ref, query_scr, block_scr = refs
    hd = LANES // 2
    rows = 2 * heads
    columns = keys_ref.shape[1]
    span = columns // heads
    whole = jnp.sum(shares_ref[...], axis=0)
    inverse = lax.rsqrt(whole[heads] / width + EPS) * 0.125
    for h in range(heads):
        query_scr[h * seqs : (h + 1) * seqs, :] = whole[h] * inverse
    base = lax.axis_index("kv") * span
    lane = lax.broadcasted_iota(jnp.int32, (rows, LANES), 1)
    sub = lax.broadcasted_iota(jnp.int32, (rows, LANES), 0)
    column = lax.broadcasted_iota(jnp.int32, (rows, columns), 1)
    row = lax.broadcasted_iota(jnp.int32, (rows, columns), 0)
    slot = lax.div(sub, heads) * heads * seqs + lax.rem(sub, heads) * seqs
    place = jnp.where(lax.rem(column, heads) == lax.rem(row, heads), column, columns)
    scores = []
    for s in range(seqs):
        one = query_scr[pl.ds(s, heads, stride=seqs), :]
        both = jnp.concatenate([one, one], axis=0)
        query = jnp.where((lane < hd) == (sub < heads), both, 0.0).astype(jnp.bfloat16)
        scores.append(
            lax.dot_general(
                query, keys_ref[s], (((1,), (1,)), ((), ())), preferred_element_type=jnp.float32
            )
        )
    weights = []
    peaks = jnp.zeros((rows, LANES), jnp.float32)
    masses = jnp.zeros((rows, LANES), jnp.float32)
    for s in range(seqs):
        used = jnp.minimum(lengths_ref[:, s : s + 1] - base, span) * heads
        valid = place < used
        masked = jnp.where(valid, scores[s], NEG)
        peak = jnp.max(masked, axis=1, keepdims=True)
        weight = jnp.where(valid, jnp.exp(masked - peak), 0.0)
        mass = jnp.sum(weight, axis=1, keepdims=True)
        weights.append(weight.astype(jnp.bfloat16))
        here = lane == slot + s
        peaks = jnp.where(here, peak, peaks)
        masses = jnp.where(here, mass, masses)
    for s in range(seqs):
        summed = jnp.dot(weights[s], values_ref[s], preferred_element_type=jnp.float32)
        for m in range(2):
            block_scr[pl.ds(m * heads * seqs + s, heads, stride=seqs), :] = summed[m * heads : (m + 1) * heads]
    parts = split3(jnp.sum(peaks, axis=0, keepdims=True)) + split3(jnp.sum(masses, axis=0, keepdims=True))
    total = seqs * rows
    tail = lax.broadcasted_iota(jnp.int32, (SUBLANES, LANES), 0)
    stats = jnp.zeros((SUBLANES, LANES), jnp.float32)
    for i, part in enumerate(parts):
        stats = jnp.where(tail == i, part, stats)
    block_scr[total : total + SUBLANES, :] = stats
    block = block_scr[...].astype(jnp.bfloat16)
    for i in range(out_ref.shape[0]):
        out_ref[i] = block


def combine_kernel(seqs, heads, blocks_ref, lambdas_ref, gain_ref, weight_ref, out_ref):
    shards = blocks_ref.shape[0]
    half = heads * seqs
    total = 2 * half
    stats = [blocks_ref[:, total + i, :].astype(jnp.float32) for i in range(6)]
    peaks = stats[0] + stats[1] + stats[2]
    masses = stats[3] + stats[4] + stats[5]
    factor = jnp.exp(peaks - jnp.max(peaks, axis=0, keepdims=True))
    mass = jnp.sum(masses * factor, axis=0, keepdims=True)
    lane = lax.broadcasted_iota(jnp.int32, (1, LANES), 1)
    sign = jnp.ones((1, LANES), jnp.float32)
    for h in range(heads):
        sign = jnp.where(lax.div(lane, seqs) == heads + h, -lambdas_ref[:, h : h + 1], sign)
    turned = jnp.transpose(factor * (sign / mass))
    summed = jnp.zeros((total, LANES), jnp.float32)
    for k in range(shards):
        summed = summed + turned[:total, k : k + 1] * blocks_ref[k, :total, :].astype(jnp.float32)
    attended = summed[:half] + summed[half:]
    norm = lax.rsqrt(jnp.mean(attended * attended, axis=1, keepdims=True) + EPS) * 0.8
    gained = (attended * gain_ref[...]).astype(jnp.bfloat16)
    part = jnp.zeros(out_ref.shape, jnp.float32)
    for h in range(heads):
        rows = slice(h * seqs, (h + 1) * seqs)
        part = part + norm[rows] * jnp.dot(
            gained[rows], weight_ref[h * LANES : (h + 1) * LANES, :], preferred_element_type=jnp.float32
        )
    out_ref[...] = part.astype(jnp.bfloat16)


def far(x):
    return pltpu.with_memory_space_constraint(x, pltpu.HBM)


def near(x):
    return pltpu.with_memory_space_constraint(x, VMEM)


def params(limit):
    return pltpu.CompilerParams(vmem_limit_bytes=limit * 1024 * 1024)


def vspec():
    return pl.BlockSpec(memory_space=VMEM)


def hspec():
    return pl.BlockSpec(memory_space=pltpu.HBM)


def exchanged(x, axis, n, distances):
    return [lax.ppermute(x, axis, [(i, i ^ d) for i in range(n)]) for d in distances]


def traded(x, axis, n):
    parts = len(ORDER)
    if n % parts:
        order = sorted(range(n), key=lambda i: i != 5 * n // 8)
    else:
        order = [part * (n // parts) + i for part in ORDER for i in range(n // parts)]
    return lax.all_to_all(x, axis, 0, 0, axis_index_groups=[order])


def body(
    n_kv,
    n_tp,
    tokens,
    norm_gain,
    query_weight,
    cache_keys,
    cache_values,
    lengths,
    lambdas,
    head_gain,
    out_weight,
):
    seqs, local = tokens.shape
    width = local * n_kv
    span, heads = cache_keys.shape[1:3]
    keys = near(cache_keys.reshape(seqs, span * heads, LANES))
    values = near(cache_values.reshape(seqs, span * heads, LANES))
    share = pl.pallas_call(
        project_kernel,
        out_shape=VMEM((n_kv, heads + 1, seqs, LANES), jnp.float32),
        in_specs=[hspec(), hspec(), hspec()],
        out_specs=vspec(),
        scratch_shapes=[
            VMEM((seqs, local), tokens.dtype),
            VMEM((1, local), norm_gain.dtype),
            VMEM(query_weight.shape, query_weight.dtype),
            pltpu.SemaphoreType.DMA((3,)),
        ],
        compiler_params=params(4),
        cost_estimate=pl.CostEstimate(flops=FLOPS, bytes_accessed=BYTES, transcendentals=0),
        name="project",
    )(far(tokens), far(norm_gain.reshape(1, local)), far(query_weight))
    shares = traded(share, "kv", n_kv)
    total = 2 * heads * seqs
    blocks = pl.pallas_call(
        functools.partial(attend_kernel, width, seqs, heads),
        out_shape=VMEM((n_kv, total + SUBLANES, LANES), jnp.bfloat16),
        in_specs=[vspec()] * 4,
        out_specs=vspec(),
        scratch_shapes=[
            VMEM((heads * seqs, LANES), jnp.float32),
            VMEM((total + SUBLANES, LANES), jnp.float32),
        ],
        compiler_params=params(16),
        name="attend",
    )(near(shares), near(lengths.reshape(1, seqs)), keys, values)
    blocks = traded(blocks, "kv", n_kv)
    part = pl.pallas_call(
        functools.partial(combine_kernel, seqs, heads),
        out_shape=VMEM((seqs, out_weight.shape[1]), jnp.bfloat16),
        in_specs=[vspec()] * 4,
        out_specs=vspec(),
        compiler_params=params(8),
        name="combine",
    )(near(blocks), near(lambdas.reshape(1, heads)), near(head_gain.reshape(1, LANES)), near(out_weight))
    if n_tp & (n_tp - 1):
        parts = list(lax.all_gather(part, "tp"))
    else:
        parts = [part] + exchanged(part, "tp", n_tp, range(1, n_tp))
    mixed = functools.reduce(jnp.add, [p.astype(jnp.float32) for p in parts])
    return mixed.astype(jnp.bfloat16)


def solution(mesh):
    in_specs = (
        P(None, "kv"),
        P("kv"),
        P("kv", "tp"),
        P(None, "kv", "tp", None),
        P(None, "kv", "tp", None),
        P(),
        P("tp"),
        P(),
        P("tp", "kv"),
    )
    step = functools.partial(body, mesh.shape["kv"], mesh.shape["tp"])
    return jax.shard_map(step, mesh=mesh, in_specs=in_specs, out_specs=P(None, "kv"), check_vma=False)
```
